256 devices in a mesh: fs: 64 (over z, x, core), tp: 4 (over y).
Axes of the slice: x: 4, y: 4, z: 8, core: 2. Of those that a mesh axis runs over, the one named last changes fastest.
Arguments:
- tokens: bfloat16 [768, 4, 2048], P(None, 'tp'), may hold values from -6 to 6
- norm_gain: float32 [2048], P('fs'), may hold values from 0.1 to 1.9
- gate_weight: float32 [8, 2048, 4096], P(None, 'fs', 'tp'), may hold values from -0.125 to 0.125
- up_weight: float32 [8, 2048, 4096], P(None, 'fs', 'tp'), may hold values from -0.125 to 0.125
- down_weight: float32 [8, 2048, 4096], P(None, 'fs', 'tp'), may hold values from -0.09375 to 0.09375
- expert_ids: int32 [768, 4, 2], P(None, 'tp'), may hold values from 0 to 7, all different within a row
- expert_mix: float32 [768, 4, 2], P(None, 'tp'), may hold values from 0.2 to 1
Outputs:
- gate_serve: bfloat16 [8, 2048, 4096], P(None, None, 'fs')
- up_serve: bfloat16 [8, 2048, 4096], P(None, None, 'fs')
- down_serve: bfloat16 [8, 2048, 4096], P(None, None, 'fs')
- mixed: bfloat16 [768, 4, 2048], P('fs', 'tp')
The draws below stay inside these ranges and needn't reach their ends.
Inputs may be any that keep to these rules, and one draw needn't show every extreme that they name: `expert_ids`: each token names two different experts.
All inputs are finite; a program needn't handle non-finite values.
Results may differ from the reference program's by a relative error of at most 0.0082.
Values may be sent and summed in bfloat16 or wider, within the bound.
No kernel may reach another device: no remote copies, remote signals or barrier semaphores. Data moves between devices by JAX's collectives and lax.ppermute only.
A program may use at most 64 MiB of HBM per device.

```python
import jax
import jax.numpy as jnp
from jax import lax

D = 2048
FF = 4096
EXPERTS = 8
ROWS = 768
N_TP = 4


def shard_levels(rng, shape, pieces, smallest, top_value):
    gain, own = 1.0, jax.random.fold_in(rng, 6)
    for axis_at, parts in pieces:
        heights = jnp.exp(jax.random.uniform(jax.random.fold_in(own, axis_at), (parts,), jnp.float32, smallest / len(pieces), top_value / len(pieces)))
        gain = gain * jnp.repeat(heights, shape[axis_at] // parts).reshape([-1 if axis == axis_at else 1 for axis in range(len(shape))])
    return gain


def picks_of(key, rows, count, top, lift):
    order = jax.random.permutation(jax.random.fold_in(key, 1), count)
    pull = order
    for power in range(3):
        pull = pull * pull // count
    pull = pull * lift // count
    tickets = jax.random.randint(jax.random.fold_in(key, 2), (rows, count), 0, 4096) + pull
    fixed_rows = jax.random.permutation(jax.random.fold_in(key, 3), rows)[jnp.arange(count) % rows]
    tickets = jnp.where(jnp.arange(rows)[:, None] == fixed_rows[None, :], 1 << 14, tickets)
    priority = tickets * count + jnp.arange(count)
    return lax.top_k(priority.astype(jnp.int32), top)[1].astype(jnp.int32)


def normal_values(rng, dims, deviation, reach, pieces=(), held_as=jnp.bfloat16):
    entries = jax.random.normal(rng, dims, jnp.float32) * deviation
    if len(pieces) > 0:
        entries = shard_levels(rng, dims, pieces, -0.22, 0.18) * entries
    return jnp.clip(entries, min=-reach, max=reach).astype(held_as)


def setup_inputs(seed: int = 0) -> dict:
    key_of = jax.random.split(jax.random.key(seed), 8)
    tokens = normal_values(key_of[0], (ROWS, N_TP, D), 1.0, 6.0, ((1, 4),))
    norm_gain = jnp.clip(1.0 + 0.18 * jax.random.normal(key_of[1], (D,), jnp.float32), 0.1, 1.9)
    gate_weight = normal_values(key_of[2], (EXPERTS, D, FF), D ** -0.5, 0.125, ((1, 64), (2, 4)), jnp.float32)
    up_weight = normal_values(key_of[3], (EXPERTS, D, FF), D ** -0.5, 0.125, ((1, 64), (2, 4)), jnp.float32)
    down_weight = normal_values(key_of[4], (EXPERTS, D, FF), FF ** -0.5, 0.09375, ((1, 64), (2, 4)), jnp.float32)
    expert_ids = picks_of(key_of[5], ROWS * N_TP, EXPERTS, 2, 0).reshape((ROWS, N_TP, 2))
    expert_mix = jnp.clip(0.2 + 0.8 * jax.random.uniform(key_of[6], (ROWS, N_TP, 2), jnp.float32) ** shard_levels(key_of[6], (ROWS, N_TP, 2), ((1, 4),), -0.2, 0.2), 0.2, 1.0)
    return dict(tokens=tokens, norm_gain=norm_gain, gate_weight=gate_weight, up_weight=up_weight, down_weight=down_weight, expert_ids=expert_ids, expert_mix=expert_mix)


norm_eps = 1e-05

def reference(tokens, norm_gain, gate_weight, up_weight, down_weight, expert_ids, expert_mix):
    gate_serve = (gate_weight * norm_gain[None, :, None]).astype(jnp.bfloat16)
    up_serve = (up_weight * norm_gain[None, :, None]).astype(jnp.bfloat16)
    down_serve = down_weight.astype(jnp.bfloat16)
    token_rows = tokens.reshape(-1, D).astype(jnp.float32)
    row_mean = lax.optimization_barrier(jnp.mean(token_rows, axis=1, keepdims=True))
    centered = token_rows - row_mean
    variance = lax.optimization_barrier(jnp.mean(centered * centered, axis=1, keepdims=True))
    normed = (centered * lax.rsqrt(variance + norm_eps)).astype(jnp.bfloat16)
    route_ids = expert_ids.reshape(-1, 2)
    route_mix = expert_mix.reshape(-1, 2)
    expert_iota = jnp.arange(EXPERTS, dtype=jnp.int32)
    expert_gates = lax.optimization_barrier(jnp.sum((route_ids[:, :, None] == expert_iota[None, None, :]).astype(jnp.float32) * route_mix[:, :, None], axis=1))

    def add_expert(running, weights_now):
        gate_mat, up_mat, down_mat, gate_col = weights_now
        gate_act = jnp.dot(normed, gate_mat, preferred_element_type=jnp.float32)
        up_act = jnp.dot(normed, up_mat, preferred_element_type=jnp.float32)
        hidden = (jax.nn.silu(gate_act) * up_act * gate_col[:, None]).astype(jnp.bfloat16)
        product = lax.dot_general(hidden, down_mat, (((1,), (1,)), ((), ())), preferred_element_type=jnp.float32)
        return (running + product, None)
    start_sum = jnp.zeros((token_rows.shape[0], D), jnp.float32)
    summed, _ = lax.scan(add_expert, start_sum, (gate_serve, up_serve, down_serve, expert_gates.T))
    mixed = summed.astype(jnp.bfloat16).reshape(ROWS, N_TP, D)
    return (gate_serve, up_serve, down_serve, mixed)
```

```python
import jax
import jax.numpy as jnp
from jax import lax
from jax.experimental import pallas as pl
from jax.experimental.pallas import tpu as pltpu
from jax.sharding import Mesh
from jax.sharding import PartitionSpec as P

FS = ("fs_0", "fs_1", "fs_2")

norm_eps = 1e-05
D_CHUNKS = 2

VMEM = pl.BlockSpec(memory_space=pltpu.VMEM)
SMEM = pl.BlockSpec(memory_space=pltpu.SMEM)


def shifted(array, axis, by):
    n = lax.axis_size(axis)
    return lax.ppermute(array, axis, [(i, (i + by) % n) for i in range(n)])


def prepare(tp_index, weight, gain):
    experts, rows, columns = weight.shape
    n_tp = lax.axis_size("tp")
    per = experts // n_tp

    def body(tp_ref, *refs):
        w_ref, outs = refs[0], refs[-n_tp:]
        low = lax.broadcasted_iota(jnp.int32, (rows, 128), 1) < 64
        if gain is not None:
            spread = jnp.broadcast_to(refs[1][...], (rows, rows))
            across = lax.broadcasted_iota(jnp.int32, (rows, rows), 1)
            down = lax.broadcasted_iota(jnp.int32, (rows, rows), 0)
            scale = jnp.sum(jnp.where(across == down, spread, 0.0), axis=1, keepdims=True)
            scale = jnp.broadcast_to(scale, (rows, 128))
        for s in range(n_tp):
            first = lax.rem(tp_ref[0] + s, n_tp) * per

            def one(pair, _, s=s, first=first):
                at = pl.ds(pl.multiple_of(pair * 128, 128), 128)
                a, b = w_ref[first, :, at], w_ref[first + 1, :, at]
                if gain is not None:
                    a, b = a * scale, b * scale
                outs[s][2 * pair] = jnp.where(low, a, pltpu.roll(b, 64, 1)).astype(jnp.bfloat16)
                outs[s][2 * pair + 1] = jnp.where(low, pltpu.roll(a, 64, 1), b).astype(jnp.bfloat16)
                return 0

            lax.fori_loop(0, columns // 128, one, 0, unroll=2)

    args = [tp_index, weight]
    if gain is not None:
        args.append(gain[None, :])
    return pl.pallas_call(
        body,
        out_shape=[jax.ShapeDtypeStruct((columns // 64, rows, 128), jnp.bfloat16)] * n_tp,
        in_specs=[SMEM] + [VMEM] * (len(args) - 1),
        out_specs=[VMEM] * n_tp,
        name="prepare",
    )(*args)


def placed(slots, blocks):
    n = len(blocks)

    def body(slot_ref, *refs):
        for i in range(n):
            refs[n][slot_ref[i]] = refs[i][...]

    return pl.pallas_call(
        body,
        out_shape=jax.ShapeDtypeStruct((n,) + blocks[0].shape, blocks[0].dtype),
        in_specs=[SMEM] + [VMEM] * n,
        out_specs=VMEM,
        name="placed",
    )(slots, *blocks)


def turned(block, chunks):
    rows = block.shape[0]
    width = rows // chunks

    def body(x_ref, *outs):
        for c in range(chunks):

            def one(i, _, c=c):
                at = pl.multiple_of(i * 256, 256)
                outs[c][:, pl.ds(at, 256)] = x_ref[pl.ds(c * width + at, 256), :].T
                return 0

            lax.fori_loop(0, width // 256, one, 0, unroll=2)

    return pl.pallas_call(
        body,
        out_shape=[jax.ShapeDtypeStruct((128, width), block.dtype)] * chunks,
        in_specs=[VMEM],
        out_specs=[VMEM] * chunks,
        name="turned",
    )(block)


def around(own):
    prev = shifted(own, "tp", 1)
    next_ = shifted(own, "tp", -1)
    low_far = shifted(prev[:64], "tp", 1)
    high_far = shifted(next_[64:], "tp", -1)
    return own, prev, next_, low_far, high_far


def joined(slots, blocks):
    def body(slot_ref, own, prev, next_, low_far, high_far, out):
        out[slot_ref[0]] = own[...]
        out[slot_ref[1]] = prev[...]
        out[slot_ref[2]] = next_[...]
        out[slot_ref[3], :64] = low_far[...]
        out[slot_ref[3], 64:] = high_far[...]

    rows, wide = blocks[0].shape
    return pl.pallas_call(
        body,
        out_shape=jax.ShapeDtypeStruct((4, rows, wide), blocks[0].dtype),
        in_specs=[SMEM] + [VMEM] * 5,
        out_specs=VMEM,
        name="joined",
    )(slots, *blocks).reshape(8, 64, wide)


def local(tokens, norm_gain, gate_weight, up_weight, down_weight, expert_ids, expert_mix):
    tp = lax.axis_index("tp").astype(jnp.int32)
    tp_index = tp.reshape(1)
    n_tp = lax.axis_size("tp")
    column_slots = jnp.stack([(tp - s) % n_tp for s in range(n_tp)])
    expert_slots = jnp.stack([tp, (tp - 1) % n_tp, (tp + 1) % n_tp, (tp + 2) % n_tp])

    def handed(weight, gain, chunks):
        blocks = prepare(tp_index, weight, gain)
        arrived = [blocks[0]]
        for s in range(1, n_tp):
            arrived.append(shifted(blocks[s], "tp", s))
        columns = placed(column_slots, arrived)
        columns = columns.reshape((-1,) + columns.shape[2:])
        mine = lax.all_to_all(columns, FS, split_axis=0, concat_axis=0, tiled=True)
        return turned(mine.reshape(-1, 128), chunks)

    (gate_own,) = handed(gate_weight, norm_gain, 1)
    (up_own,) = handed(up_weight, norm_gain, 1)
    down_own = handed(down_weight, None, D_CHUNKS)

    width = tokens.shape[2]
    count = tokens.shape[0]
    n_z, n_x, n_c = (lax.axis_size(a) for a in FS)
    own_rows = count // (n_z * n_x * n_c)
    row = jnp.arange(count, dtype=jnp.int32)
    c_at = (row // (count // n_c) + lax.axis_index("fs_2")) % n_c
    x_at = (row // (count // n_c // n_x) + lax.axis_index("fs_1")) % n_x
    z_at = (row // own_rows) % n_z
    source = ((z_at * n_x + x_at) * n_c + c_at) * own_rows + row % own_rows
    pick = source[:, None] == row[None, :]

    token_rows = tokens.reshape(count, width).astype(jnp.float32)
    row_mean = jnp.mean(token_rows, axis=1, keepdims=True)
    centered = token_rows - row_mean
    variance = jnp.mean(centered * centered, axis=1, keepdims=True)
    normed = (centered * lax.rsqrt(variance + norm_eps)).astype(jnp.bfloat16)
    normed = jnp.dot(pick.astype(jnp.bfloat16), normed, preferred_element_type=jnp.float32)
    normed = normed.astype(jnp.bfloat16)
    route_ids = expert_ids.reshape(-1, 2)
    route_mix = expert_mix.reshape(-1, 2)
    experts = gate_weight.shape[0]
    expert_iota = jnp.arange(experts, dtype=jnp.int32)
    expert_gates = jnp.sum(
        (route_ids[:, :, None] == expert_iota[None, None, :]).astype(jnp.float32)
        * route_mix[:, :, None],
        axis=1,
    )
    expert_gates = jnp.dot(
        pick.astype(jnp.float32), expert_gates, precision=lax.Precision.HIGHEST
    )

    contract = (((1,), (1,)), ((), ()))
    gate_all = joined(expert_slots, around(gate_own))
    up_all = joined(expert_slots, around(up_own))
    units = gate_all.shape[1]
    gate_act = lax.dot_general(
        normed, gate_all.reshape(-1, width), contract, preferred_element_type=jnp.float32
    )
    up_act = lax.dot_general(
        normed, up_all.reshape(-1, width), contract, preferred_element_type=jnp.float32
    )
    hidden = jax.nn.silu(gate_act) * up_act * jnp.repeat(expert_gates, units, axis=1)
    hidden = hidden.astype(jnp.bfloat16)

    down_parts, mixed_parts = [], []
    half, quarter = count // n_c, count // n_c // n_x
    for c in range(D_CHUNKS):
        down_c = joined(expert_slots, around(down_own[c]))
        down_parts.append(down_c)
        wide = down_c.shape[2]
        part = jnp.dot(hidden, down_c.reshape(-1, wide), preferred_element_type=jnp.float32)
        sent = shifted(part[half:].astype(jnp.bfloat16), "fs_2", 1)
        part = part[:half] + sent.astype(jnp.float32)
        total = part[:quarter]
        for s in range(1, n_x):
            block = part[s * quarter : (s + 1) * quarter].astype(jnp.bfloat16)
            block = shifted(block, "fs_1", s)
            total = total + block.astype(jnp.float32)
        block = total.astype(jnp.bfloat16).reshape(n_z, own_rows, wide)
        block = lax.all_to_all(block, "fs_0", split_axis=0, concat_axis=0, tiled=True)
        mixed_parts.append(jnp.sum(block.astype(jnp.float32), axis=0).astype(jnp.bfloat16))
    down_all = jnp.concatenate(down_parts, axis=2)
    mixed = jnp.concatenate(mixed_parts, axis=1)[:, None, :]

    def as_served(a):
        return jnp.transpose(a, (0, 2, 1))

    return (as_served(gate_all), as_served(up_all), as_served(down_all), mixed)


def solution(mesh):
    finer = Mesh(mesh.devices.reshape(8, 4, 2, mesh.shape["tp"]), ("fs_0", "fs_1", "fs_2", "tp"))
    placed_as = (
        P(None, "tp", None),
        P(FS),
        P(None, FS, "tp"),
        P(None, FS, "tp"),
        P(None, FS, "tp"),
        P(None, "tp", None),
        P(None, "tp", None),
    )
    return jax.shard_map(
        local,
        mesh=finer,
        in_specs=placed_as,
        out_specs=(P(None, None, FS), P(None, None, FS), P(None, None, FS), P(FS, "tp", None)),
        check_vma=False,
    )
```

```python
import jax
import jax.numpy as jnp
from jax import lax
from jax.experimental import pallas as pl
from jax.experimental.pallas import tpu as pltpu
from jax.sharding import Mesh
from jax.sharding import PartitionSpec as P

FS = ("fs_0", "fs_1", "fs_2")
VMEM_LIMIT = pltpu.CompilerParams(vmem_limit_bytes=16 << 20)

norm_eps = 1e-05
D_WIDTHS = (1024, 1024)
RELAYED = {"g": 1, "u": -1}

VMEM = pl.BlockSpec(memory_space=pltpu.VMEM)
SMEM = pl.BlockSpec(memory_space=pltpu.SMEM)


def shifted(array, axis, by):
    n = lax.axis_size(axis)
    return lax.ppermute(array, axis, [(i, (i + by) % n) for i in range(n)])


def prepare(tp_index, gain, weights, scaled):
    experts, rows, columns = weights[0].shape
    n_tp = lax.axis_size("tp")
    per = experts // n_tp
    n = len(weights)

    def body(tp_ref, gain_ref, *refs):
        outs = refs[n:]
        low = lax.broadcasted_iota(jnp.int32, (rows, 128), 1) < 64
        spread = jnp.broadcast_to(gain_ref[...], (rows, rows))
        across = lax.broadcasted_iota(jnp.int32, (rows, rows), 1)
        down = lax.broadcasted_iota(jnp.int32, (rows, rows), 0)
        scale = jnp.sum(jnp.where(across == down, spread, 0.0), axis=1, keepdims=True)
        scale = jnp.broadcast_to(scale, (rows, 128))
        for s in range(n_tp):
            first = lax.rem(tp_ref[0] + s, n_tp) * per

            def one(pair, _, s=s, first=first):
                at = pl.ds(pl.multiple_of(pair * 128, 128), 128)
                for m in range(n):
                    a, b = refs[m][first, :, at], refs[m][first + 1, :, at]
                    if scaled[m]:
                        a, b = a * scale, b * scale
                    even = jnp.where(low, a, pltpu.roll(b, 64, 1))
                    odd = jnp.where(low, pltpu.roll(a, 64, 1), b)
                    outs[s][2 * pair, m] = even.astype(jnp.bfloat16)
                    outs[s][2 * pair + 1, m] = odd.astype(jnp.bfloat16)
                return 0

            lax.fori_loop(0, columns // 128, one, 0, unroll=2)

    return pl.pallas_call(
        body,
        out_shape=[jax.ShapeDtypeStruct((columns // 64, n, rows, 128), jnp.bfloat16)] * n_tp,
        in_specs=[SMEM] + [VMEM] * (n + 1),
        out_specs=[VMEM] * n_tp,
        compiler_params=VMEM_LIMIT,
        name="prepare",
    )(tp_index, gain[None, :], *weights)


def placed(slots, blocks):
    n = len(blocks)

    def body(slot_ref, *refs):
        for i in range(n):
            refs[n][slot_ref[i]] = refs[i][...]

    return pl.pallas_call(
        body,
        out_shape=jax.ShapeDtypeStruct((n,) + blocks[0].shape, blocks[0].dtype),
        in_specs=[SMEM] + [VMEM] * n,
        out_specs=VMEM,
        compiler_params=VMEM_LIMIT,
        name="placed",
    )(slots, *blocks)


def fill(slot_ref, refs, all_ref):
    for i, ref in enumerate(refs):
        at = pl.multiple_of(slot_ref[i] * 64, 64)
        all_ref[pl.ds(at, ref.shape[0]), :] = ref[...]


def acted(slots, normed, blocks, gate_act=None, gates=None):
    tokens, width = normed.shape
    n = len(blocks)
    units = 512
    step = tokens // 2
    last = gate_act is not None

    def body(slot_ref, n_ref, *refs):
        all_ref, out_ref = refs[-2:]
        fill(slot_ref, refs[:n], all_ref)
        low = lax.broadcasted_iota(jnp.int32, (step, 128), 1) < 64

        def one(i, _):
            rows = pl.ds(pl.multiple_of(i * step, step), step)
            for at in range(0, units, 256):
                act = lax.dot_general(
                    n_ref[rows, :],
                    all_ref[pl.ds(at, 256), :],
                    (((1,), (1,)), ((), ())),
                    preferred_element_type=jnp.float32,
                )
                if not last:
                    out_ref[rows, pl.ds(at, 256)] = act
                    continue
                for half in range(2):
                    cols = pl.ds(at + half * 128, 128)
                    e = (at + half * 128) // 64
                    mix = jnp.where(
                        low, refs[n + 1][rows, e : e + 1], refs[n + 1][rows, e + 1 : e + 2]
                    )
                    up = act[:, half * 128 : (half + 1) * 128]
                    hidden = jax.nn.silu(refs[n][rows, cols]) * up * mix
                    out_ref[rows, cols] = hidden.astype(jnp.bfloat16)
            return 0

        lax.fori_loop(0, 2, one, 0)

    args = [slots, normed, *blocks] + ([gate_act, gates] if last else [])
    return pl.pallas_call(
        body,
        out_shape=[
            jax.ShapeDtypeStruct((units, width), jnp.bfloat16),
            jax.ShapeDtypeStruct((tokens, units), jnp.bfloat16 if last else jnp.float32),
        ],
        in_specs=[SMEM] + [VMEM] * (len(args) - 1),
        out_specs=[VMEM] * 2,
        compiler_params=pltpu.CompilerParams(vmem_limit_bytes=24 << 20),
        name="acted",
    )(*args)


def turned(block, widths):
    _, n, rows, lanes = block.shape
    step = 256 // rows
    outs = [(m, w) for m in range(n) for w in widths]

    def body(x_ref, *refs):
        for k, (m, width) in enumerate(outs):
            start = sum(w for p, w in outs[:k] if p == m) // rows

            def one(i, _, out=refs[k], m=m, start=start):
                t = x_ref[pl.ds(start + i * step, step), m].reshape(256, lanes).T
                out[:, pl.ds(pl.multiple_of(i * 256, 256), 256)] = t
                return 0

            lax.fori_loop(0, width // 256, one, 0)

    return pl.pallas_call(
        body,
        out_shape=[jax.ShapeDtypeStruct((lanes, w), block.dtype) for _, w in outs],
        in_specs=[VMEM],
        out_specs=[VMEM] * len(outs),
        compiler_params=VMEM_LIMIT,
        name="turned",
    )(block)


def gathered(name, own):
    n_tp = lax.axis_size("tp")
    tp = lax.axis_index("tp").astype(jnp.int32)

    def sent(block, by):
        return shifted(block, "tp", by)

    prev, after = sent(own, 1), sent(own, -1)
    slots = [2 * tp, 2 * ((tp - 1) % n_tp), 2 * ((tp + 1) % n_tp), 2 * ((tp + 2) % n_tp)]
    if name in RELAYED:
        far = [sent(*((prev, 1) if RELAYED[name] > 0 else (after, -1)))]
    else:
        far = [sent(own, 2)]
    return jnp.stack(slots), [own, prev, after] + far


def mixed_away(slots, hidden, blocks):
    tokens, units = hidden.shape
    half = tokens // 2
    wide = blocks[0].shape[1]
    n = len(blocks)

    def body(slot_ref, h_ref, *refs):
        all_ref, away_ref = refs[n:]
        fill(slot_ref, refs[:n], all_ref)

        def one(i, _):
            at = pl.ds(pl.multiple_of(i * 256, 256), 256)
            part = jnp.dot(h_ref[half:], all_ref[:, at], preferred_element_type=jnp.float32)
            away_ref[:, at] = part.astype(jnp.bfloat16)
            return 0

        lax.fori_loop(0, wide // 256, one, 0)

    return pl.pallas_call(
        body,
        out_shape=[
            jax.ShapeDtypeStruct((units, wide), jnp.bfloat16),
            jax.ShapeDtypeStruct((half, wide), jnp.bfloat16),
        ],
        in_specs=[SMEM] + [VMEM] * (n + 1),
        out_specs=[VMEM] * 2,
        compiler_params=VMEM_LIMIT,
        name="mixed_away",
    )(slots, hidden, *blocks)


def mixed_here(hidden, down, arrived, n_x):
    half, wide = arrived.shape
    rows = half // n_x

    def body(h_ref, d_ref, r_ref, *outs):
        def one(i, _):
            at = pl.ds(pl.multiple_of(i * 256, 256), 256)
            part = jnp.dot(h_ref[:half], d_ref[:, at], preferred_element_type=jnp.float32)
            part = part + r_ref[:, at].astype(jnp.float32)
            for x in range(n_x):
                outs[x][:, at] = part[x * rows : (x + 1) * rows].astype(outs[x].dtype)
            return 0

        lax.fori_loop(0, wide // 256, one, 0)

    return pl.pallas_call(
        body,
        out_shape=[
            jax.ShapeDtypeStruct((rows, wide), jnp.bfloat16 if x else jnp.float32)
            for x in range(n_x)
        ],
        in_specs=[VMEM] * 3,
        out_specs=[VMEM] * n_x,
        compiler_params=VMEM_LIMIT,
        name="mixed_here",
    )(hidden, down, arrived)


def folded(parts, n_z):
    widths = [p[0].shape[1] for p in parts]
    count = parts[0][0].shape[0]
    width = sum(widths)
    rows, half = count // n_z, width // 2
    flat = [a for p in parts for a in p]
    per = len(parts[0])

    def body(*refs):
        out, total = refs[-2:]
        start = 0
        for c, wide in enumerate(widths):
            part = refs[c * per][...]
            for i in range(1, per):
                part = part + refs[c * per + i][...].astype(jnp.float32)
            total[:, pl.ds(start, wide)] = part
            start += wide
        for z in range(n_z):
            at = pl.ds(z * rows, rows)
            piece = jnp.concatenate([total[at, :half], total[at, half:]], axis=0)
            out[z] = piece.astype(out.dtype)

    return pl.pallas_call(
        body,
        out_shape=jax.ShapeDtypeStruct((n_z, 2 * rows, half), jnp.bfloat16),
        in_specs=[VMEM] * len(flat),
        out_specs=VMEM,
        scratch_shapes=[pltpu.VMEM((count, width), jnp.float32)],
        compiler_params=VMEM_LIMIT,
        name="folded",
    )(*flat)


def finished(pieces):
    n_z, rows, half = pieces.shape

    def body(p_ref, out):
        total = p_ref[0].astype(jnp.float32)
        for z in range(1, n_z):
            total = total + p_ref[z].astype(jnp.float32)
        wide = jnp.concatenate([total[: rows // 2], total[rows // 2 :]], axis=1)
        out[...] = wide.astype(jnp.bfloat16)

    return pl.pallas_call(
        body,
        out_shape=jax.ShapeDtypeStruct((rows // 2, 2 * half), jnp.bfloat16),
        in_specs=[VMEM],
        out_specs=VMEM,
        compiler_params=VMEM_LIMIT,
        name="finished",
    )(pieces)


def local(tokens, norm_gain, gate_weight, up_weight, down_weight, expert_ids, expert_mix):
    tp = lax.axis_index("tp").astype(jnp.int32)
    tp_index = tp.reshape(1)
    n_tp = lax.axis_size("tp")
    column_slots = jnp.stack([(tp - s) % n_tp for s in range(n_tp)])

    def handed(weights, scaled):
        blocks = prepare(tp_index, norm_gain, weights, scaled)
        arrived = [blocks[0]]
        for s in range(1, n_tp):
            arrived.append(shifted(blocks[s], "tp", s))
        columns = placed(column_slots, arrived)
        columns = columns.reshape((-1,) + columns.shape[2:])
        return lax.all_to_all(columns, FS, split_axis=0, concat_axis=0, tiled=True)

    block_a = handed((gate_weight, up_weight), (True, True))
    block_d = handed((down_weight,), (False,))
    gate_own, up_own = turned(block_a, (tokens.shape[2],))
    down_own = turned(block_d, D_WIDTHS)
    gate_pieces = gathered("g", gate_own)
    up_pieces = gathered("u", up_own)
    down_pieces = [gathered(f"d{c}", own) for c, own in enumerate(down_own)]

    width = tokens.shape[2]
    count = tokens.shape[0]
    n_z, n_x, n_c = (lax.axis_size(a) for a in FS)
    own_rows = count // (n_z * n_x * n_c)
    row = jnp.arange(count, dtype=jnp.int32)
    c_at = (row // (count // n_c) + lax.axis_index("fs_2")) % n_c
    x_at = (row // (count // n_c // n_x) + lax.axis_index("fs_1")) % n_x
    z_at = (row // own_rows) % n_z
    source = ((z_at * n_x + x_at) * n_c + c_at) * own_rows + row % own_rows
    pick = source[:, None] == row[None, :]

    token_rows = tokens.reshape(count, width).astype(jnp.float32)
    row_mean = jnp.mean(token_rows, axis=1, keepdims=True)
    centered = token_rows - row_mean
    variance = jnp.mean(centered * centered, axis=1, keepdims=True)
    normed = (centered * lax.rsqrt(variance + norm_eps)).astype(jnp.bfloat16)
    normed = jnp.dot(pick.astype(jnp.bfloat16), normed, preferred_element_type=jnp.float32)
    normed = normed.astype(jnp.bfloat16)
    route_ids = expert_ids.reshape(-1, 2)
    route_mix = expert_mix.reshape(-1, 2)
    experts = gate_weight.shape[0]
    expert_iota = jnp.arange(experts, dtype=jnp.int32)
    expert_gates = jnp.sum(
        (route_ids[:, :, None] == expert_iota[None, None, :]).astype(jnp.float32)
        * route_mix[:, :, None],
        axis=1,
    )
    expert_gates = jnp.dot(pick.astype(jnp.float32), expert_gates, precision=lax.Precision.HIGHEST)

    gate_all, gate_act = acted(gate_pieces[0], normed, gate_pieces[1])
    up_all, hidden = acted(up_pieces[0], normed, up_pieces[1], gate_act, expert_gates)
    units = up_all.shape[0] // experts

    down_parts, summed = [], []
    for slots, pieces in down_pieces:
        down_c, away = mixed_away(slots, hidden, pieces)
        down_parts.append(down_c)
        away = shifted(away, "fs_2", 1)
        blocks = list(mixed_here(hidden, down_c, away, n_x))
        for s in range(1, n_x):
            blocks[s] = shifted(blocks[s], "fs_1", s)
        summed.append(blocks)
    pieces = folded(summed, n_z)
    pieces = lax.all_to_all(pieces, "fs_0", split_axis=0, concat_axis=0, tiled=True)
    mixed = finished(pieces)[:, None, :]
    down_all = jnp.concatenate(down_parts, axis=1)

    def as_served(a):
        return jnp.transpose(a.reshape(experts, units, width), (0, 2, 1))

    return (as_served(gate_all), as_served(up_all), as_served(down_all), mixed)


def solution(mesh):
    finer = Mesh(mesh.devices.reshape(8, 4, 2, mesh.shape["tp"]), ("fs_0", "fs_1", "fs_2", "tp"))
    placed_as = (
        P(None, "tp", None),
        P(FS),
        P(None, FS, "tp"),
        P(None, FS, "tp"),
        P(None, FS, "tp"),
        P(None, "tp", None),
        P(None, "tp", None),
    )
    return jax.shard_map(
        local,
        mesh=finer,
        in_specs=placed_as,
        out_specs=(P(None, None, FS), P(None, None, FS), P(None, None, FS), P(FS, "tp", None)),
        check_vma=False,
    )
```

```python
import jax
import jax.numpy as jnp
from jax import lax
from jax.experimental import pallas as pl
from jax.experimental.pallas import tpu as pltpu
from jax.sharding import Mesh
from jax.sharding import PartitionSpec as P

FS = ("fs_0", "fs_1", "fs_2")
VMEM_LIMIT = pltpu.CompilerParams(vmem_limit_bytes=16 << 20)

norm_eps = 1e-05
D_WIDTHS = (1024, 1024)
RELAYED = {"g": 1, "u": -1}

VMEM = pl.BlockSpec(memory_space=pltpu.VMEM)
SMEM = pl.BlockSpec(memory_space=pltpu.SMEM)


def shifted(array, axis, by):
    n = lax.axis_size(axis)
    return lax.ppermute(array, axis, [(i, (i + by) % n) for i in range(n)])


def prepare(tp_index, gain, weights, scaled):
    experts, rows, columns = weights[0].shape
    n_tp = lax.axis_size("tp")
    per = experts // n_tp
    n = len(weights)

    def body(tp_ref, gain_ref, *refs):
        outs = refs[n:]
        low = lax.broadcasted_iota(jnp.int32, (rows, 128), 1) < 64
        spread = jnp.broadcast_to(gain_ref[...], (rows, rows))
        across = lax.broadcasted_iota(jnp.int32, (rows, rows), 1)
        down = lax.broadcasted_iota(jnp.int32, (rows, rows), 0)
        scale = jnp.sum(jnp.where(across == down, spread, 0.0), axis=1, keepdims=True)
        scale = jnp.broadcast_to(scale, (rows, 128))
        for s in range(n_tp):
            first = lax.rem(tp_ref[0] + s, n_tp) * per

            def one(pair, _, s=s, first=first):
                at = pl.ds(pl.multiple_of(pair * 128, 128), 128)
                for m in range(n):
                    a, b = refs[m][first, :, at], refs[m][first + 1, :, at]
                    if scaled[m]:
                        a, b = a * scale, b * scale
                    even = jnp.where(low, a, pltpu.roll(b, 64, 1))
                    odd = jnp.where(low, pltpu.roll(a, 64, 1), b)
                    outs[s][2 * pair, m] = even.astype(jnp.bfloat16)
                    outs[s][2 * pair + 1, m] = odd.astype(jnp.bfloat16)
                return 0

            lax.fori_loop(0, columns // 128, one, 0, unroll=2)

    return pl.pallas_call(
        body,
        out_shape=[jax.ShapeDtypeStruct((columns // 64, n, rows, 128), jnp.bfloat16)] * n_tp,
        in_specs=[SMEM] + [VMEM] * (n + 1),
        out_specs=[VMEM] * n_tp,
        compiler_params=VMEM_LIMIT,
        name="prepare",
    )(tp_index, gain[None, :], *weights)


def placed(tp_index, blocks):
    n = len(blocks)

    def body(tp_ref, *refs):
        for s in range(n):
            refs[n][lax.rem(tp_ref[0] + (n - s), n)] = refs[s][...]

    return pl.pallas_call(
        body,
        out_shape=jax.ShapeDtypeStruct((n,) + blocks[0].shape, blocks[0].dtype),
        in_specs=[SMEM] + [VMEM] * n,
        out_specs=VMEM,
        compiler_params=VMEM_LIMIT,
        name="placed",
    )(tp_index, *blocks)


def fill(tp_ref, refs, all_ref):
    rows = refs[0].shape[0]
    for ref, ahead in zip(refs, (0, 3, 1, 2)):
        at = pl.multiple_of(lax.rem(tp_ref[0] + ahead, 4) * rows, rows)
        all_ref[pl.ds(at, rows), :] = ref[...]


def acted(tp_index, normed, blocks, gate_act=None, gates=None):
    tokens, width = normed.shape
    n = len(blocks)
    units = 512
    step = tokens // 2
    last = gate_act is not None

    def body(tp_ref, n_ref, *refs):
        all_ref, out_ref = refs[-2:]
        fill(tp_ref, refs[:n], all_ref)
        low = lax.broadcasted_iota(jnp.int32, (step, 128), 1) < 64

        def one(i, _):
            rows = pl.ds(pl.multiple_of(i * step, step), step)
            for at in range(0, units, 256):
                act = lax.dot_general(
                    n_ref[rows, :],
                    all_ref[pl.ds(at, 256), :],
                    (((1,), (1,)), ((), ())),
                    preferred_element_type=jnp.float32,
                )
                if not last:
                    out_ref[rows, pl.ds(at, 256)] = act
                    continue
                for half in range(2):
                    cols = pl.ds(at + half * 128, 128)
                    e = (at + half * 128) // 64
                    mix = jnp.where(
                        low, refs[n + 1][rows, e : e + 1], refs[n + 1][rows, e + 1 : e + 2]
                    )
                    up = act[:, half * 128 : (half + 1) * 128]
                    hidden = jax.nn.silu(refs[n][rows, cols]) * up * mix
                    out_ref[rows, cols] = hidden.astype(jnp.bfloat16)
            return 0

        lax.fori_loop(0, 2, one, 0)

    args = [tp_index, normed, *blocks] + ([gate_act, gates] if last else [])
    return pl.pallas_call(
        body,
        out_shape=[
            jax.ShapeDtypeStruct((units, width), jnp.bfloat16),
            jax.ShapeDtypeStruct((tokens, units), jnp.bfloat16 if last else jnp.float32),
        ],
        in_specs=[SMEM] + [VMEM] * (len(args) - 1),
        out_specs=[VMEM] * 2,
        compiler_params=pltpu.CompilerParams(vmem_limit_bytes=24 << 20),
        name="acted",
    )(*args)


def turned(block, widths):
    _, n, rows, lanes = block.shape
    step = 256 // rows
    outs = [(m, w) for m in range(n) for w in widths]

    def body(x_ref, *refs):
        for k, (m, width) in enumerate(outs):
            start = sum(w for p, w in outs[:k] if p == m) // rows

            def one(i, _, out=refs[k], m=m, start=start):
                t = x_ref[pl.ds(start + i * step, step), m].reshape(256, lanes).T
                out[:, pl.ds(pl.multiple_of(i * 256, 256), 256)] = t
                return 0

            lax.fori_loop(0, width // 256, one, 0)

    return pl.pallas_call(
        body,
        out_shape=[jax.ShapeDtypeStruct((lanes, w), block.dtype) for _, w in outs],
        in_specs=[VMEM],
        out_specs=[VMEM] * len(outs),
        compiler_params=VMEM_LIMIT,
        name="turned",
    )(block)


def gathered(name, own):

    def sent(block, by):
        return shifted(block, "tp", by)

    prev, after = sent(own, 1), sent(own, -1)
    if name in RELAYED:
        far = [sent(*((prev, 1) if RELAYED[name] > 0 else (after, -1)))]
    else:
        far = [sent(own, 2)]
    return [own, prev, after] + far


def mixed_away(tp_index, hidden, blocks):
    tokens, units = hidden.shape
    half = tokens // 2
    wide = blocks[0].shape[1]
    n = len(blocks)

    def body(tp_ref, h_ref, *refs):
        all_ref, away_ref = refs[n:]
        fill(tp_ref, refs[:n], all_ref)

        def one(i, _):
            at = pl.ds(pl.multiple_of(i * 256, 256), 256)
            part = jnp.dot(h_ref[half:], all_ref[:, at], preferred_element_type=jnp.float32)
            away_ref[:, at] = part.astype(jnp.bfloat16)
            return 0

        lax.fori_loop(0, wide // 256, one, 0)

    return pl.pallas_call(
        body,
        out_shape=[
            jax.ShapeDtypeStruct((units, wide), jnp.bfloat16),
            jax.ShapeDtypeStruct((half, wide), jnp.bfloat16),
        ],
        in_specs=[SMEM] + [VMEM] * (n + 1),
        out_specs=[VMEM] * 2,
        compiler_params=VMEM_LIMIT,
        name="mixed_away",
    )(tp_index, hidden, *blocks)


def mixed_here(hidden, down, arrived, n_x):
    half, wide = arrived.shape
    rows = half // n_x

    def body(h_ref, d_ref, r_ref, *outs):
        def one(i, _):
            at = pl.ds(pl.multiple_of(i * 256, 256), 256)
            part = jnp.dot(h_ref[:half], d_ref[:, at], preferred_element_type=jnp.float32)
            part = part + r_ref[:, at].astype(jnp.float32)
            for x in range(n_x):
                outs[x][:, at] = part[x * rows : (x + 1) * rows].astype(outs[x].dtype)
            return 0

        lax.fori_loop(0, wide // 256, one, 0)

    return pl.pallas_call(
        body,
        out_shape=[
            jax.ShapeDtypeStruct((rows, wide), jnp.bfloat16 if x else jnp.float32)
            for x in range(n_x)
        ],
        in_specs=[VMEM] * 3,
        out_specs=[VMEM] * n_x,
        compiler_params=VMEM_LIMIT,
        name="mixed_here",
    )(hidden, down, arrived)


def folded(parts, n_z):
    widths = [p[0].shape[1] for p in parts]
    count = parts[0][0].shape[0]
    width = sum(widths)
    rows, half = count // n_z, width // 2
    flat = [a for p in parts for a in p]
    per = len(parts[0])

    def body(*refs):
        outs, total = refs[len(flat) : -1], refs[-1]
        start = 0
        for c, wide in enumerate(widths):
            part = refs[c * per][...]
            for i in range(1, per):
                part = part + refs[c * per + i][...].astype(jnp.float32)
            total[:, pl.ds(start, wide)] = part
            start += wide
        for z in range(n_z):
            at = pl.ds(z * rows, rows)
            piece = jnp.concatenate([total[at, :half], total[at, half:]], axis=0)
            outs[z][...] = piece.astype(outs[z].dtype)

    return pl.pallas_call(
        body,
        out_shape=[
            jax.ShapeDtypeStruct((2 * rows, half), jnp.bfloat16 if z else jnp.float32)
            for z in range(n_z)
        ],
        in_specs=[VMEM] * len(flat),
        out_specs=[VMEM] * n_z,
        scratch_shapes=[pltpu.VMEM((count, width), jnp.float32)],
        compiler_params=VMEM_LIMIT,
        name="folded",
    )(*flat)


def finished(pieces):
    rows, half = pieces[0].shape

    def body(*refs):
        total = refs[0][...]
        for r in refs[1:-1]:
            total = total + r[...].astype(jnp.float32)
        refs[-1][:, :half] = total[: rows // 2].astype(jnp.bfloat16)
        refs[-1][:, half:] = total[rows // 2 :].astype(jnp.bfloat16)

    return pl.pallas_call(
        body,
        out_shape=jax.ShapeDtypeStruct((rows // 2, 2 * half), jnp.bfloat16),
        in_specs=[VMEM] * len(pieces),
        out_specs=VMEM,
        compiler_params=VMEM_LIMIT,
        name="finished",
    )(*pieces)


def side_by_side(parts):
    rows = parts[0].shape[0]
    widths = [p.shape[1] for p in parts]

    def body(*refs):
        for i, ref in enumerate(refs[:-1]):
            refs[-1][:, pl.ds(sum(widths[:i]), widths[i])] = ref[...]

    return pl.pallas_call(
        body,
        out_shape=jax.ShapeDtypeStruct((rows, sum(widths)), parts[0].dtype),
        in_specs=[VMEM] * len(parts),
        out_specs=VMEM,
        compiler_params=VMEM_LIMIT,
        name="side_by_side",
    )(*parts)


def local(tokens, norm_gain, gate_weight, up_weight, down_weight, expert_ids, expert_mix):
    tp = lax.axis_index("tp").astype(jnp.int32)
    tp_index = tp.reshape(1)
    n_tp = lax.axis_size("tp")

    def handed(weights, scaled):
        blocks = prepare(tp_index, norm_gain, weights, scaled)
        arrived = [blocks[0]]
        for s in range(1, n_tp):
            arrived.append(shifted(blocks[s], "tp", s))
        columns = placed(tp_index, arrived)
        columns = columns.reshape((-1,) + columns.shape[2:])
        return lax.all_to_all(columns, FS, split_axis=0, concat_axis=0, tiled=True)

    block_a = handed((gate_weight, up_weight), (True, True))
    block_d = handed((down_weight,), (False,))
    gate_own, up_own = turned(block_a, (tokens.shape[2],))
    down_own = turned(block_d, D_WIDTHS)
    gate_pieces = gathered("g", gate_own)
    up_pieces = gathered("u", up_own)
    down_pieces = [gathered(f"d{c}", own) for c, own in enumerate(down_own)]

    width = tokens.shape[2]
    count = tokens.shape[0]
    n_z, n_x, n_c = (lax.axis_size(a) for a in FS)
    own_rows = count // (n_z * n_x * n_c)
    row = jnp.arange(count, dtype=jnp.int32)
    c_at = (row // (count // n_c) + lax.axis_index("fs_2")) % n_c
    x_at = (row // (count // n_c // n_x) + lax.axis_index("fs_1")) % n_x
    z_at = (row // own_rows + lax.axis_index("fs_0")) % n_z
    source = ((z_at * n_x + x_at) * n_c + c_at) * own_rows + row % own_rows
    pick = source[:, None] == row[None, :]

    token_rows = tokens.reshape(count, width).astype(jnp.float32)
    row_mean = jnp.mean(token_rows, axis=1, keepdims=True)
    centered = token_rows - row_mean
    variance = jnp.mean(centered * centered, axis=1, keepdims=True)
    normed = (centered * lax.rsqrt(variance + norm_eps)).astype(jnp.bfloat16)
    normed = jnp.dot(pick.astype(jnp.bfloat16), normed, preferred_element_type=jnp.float32)
    normed = normed.astype(jnp.bfloat16)
    route_ids = expert_ids.reshape(-1, 2)
    route_mix = expert_mix.reshape(-1, 2)
    experts = gate_weight.shape[0]
    expert_iota = jnp.arange(experts, dtype=jnp.int32)
    expert_gates = jnp.sum(
        (route_ids[:, :, None] == expert_iota[None, None, :]).astype(jnp.float32)
        * route_mix[:, :, None],
        axis=1,
    )
    expert_gates = jnp.dot(pick.astype(jnp.float32), expert_gates, precision=lax.Precision.HIGHEST)

    gate_all, gate_act = acted(tp_index, normed, gate_pieces)
    up_all, hidden = acted(tp_index, normed, up_pieces, gate_act, expert_gates)
    units = up_all.shape[0] // experts

    down_parts, summed = [], []
    for pieces in down_pieces:
        down_c, away = mixed_away(tp_index, hidden, pieces)
        down_parts.append(down_c)
        away = shifted(away, "fs_2", 1)
        blocks = list(mixed_here(hidden, down_c, away, n_x))
        for s in range(1, n_x):
            blocks[s] = shifted(blocks[s], "fs_1", s)
        summed.append(blocks)
    pieces = list(folded(summed, n_z))
    for s in range(1, n_z):
        pieces[s] = shifted(pieces[s], "fs_0", s)
    mixed = finished(pieces)[:, None, :]
    down_all = side_by_side(down_parts)

    def as_served(a):
        return jnp.transpose(a.reshape(experts, units, width), (0, 2, 1))

    return (as_served(gate_all), as_served(up_all), as_served(down_all), mixed)


def solution(mesh):
    finer = Mesh(mesh.devices.reshape(8, 4, 2, mesh.shape["tp"]), ("fs_0", "fs_1", "fs_2", "tp"))
    placed_as = (
        P(None, "tp", None),
        P(FS),
        P(None, FS, "tp"),
        P(None, FS, "tp"),
        P(None, FS, "tp"),
        P(None, "tp", None),
        P(None, "tp", None),
    )
    return jax.shard_map(
        local,
        mesh=finer,
        in_specs=placed_as,
        out_specs=(P(None, None, FS), P(None, None, FS), P(None, None, FS), P(FS, "tp", None)),
        check_vma=False,
    )
```

```python
import jax
import jax.numpy as jnp
from jax import lax
from jax.experimental import pallas as pl
from jax.experimental.pallas import tpu as pltpu
from jax.sharding import Mesh
from jax.sharding import PartitionSpec as P

FS = ("fs_0", "fs_1", "fs_2")
VMEM_LIMIT = pltpu.CompilerParams(vmem_limit_bytes=16 << 20)

norm_eps = 1e-05
D_WIDTHS = (1024, 1024)
RELAYED = {"g": 1, "u": -1}

VMEM = pl.BlockSpec(memory_space=pltpu.VMEM)
SMEM = pl.BlockSpec(memory_space=pltpu.SMEM)


def shifted(array, axis, by):
    n = lax.axis_size(axis)
    return lax.ppermute(array, axis, [(i, (i + by) % n) for i in range(n)])


def prepare(tp_index, gain, weights, scaled):
    experts, rows, columns = weights[0].shape
    n_tp = lax.axis_size("tp")
    per = experts // n_tp
    n = len(weights)

    def body(tp_ref, gain_ref, *refs):
        outs = refs[n:]
        low = lax.broadcasted_iota(jnp.int32, (rows, 128), 1) < 64
        spread = jnp.broadcast_to(gain_ref[...], (rows, rows))
        across = lax.broadcasted_iota(jnp.int32, (rows, rows), 1)
        down = lax.broadcasted_iota(jnp.int32, (rows, rows), 0)
        scale = jnp.sum(jnp.where(across == down, spread, 0.0), axis=1, keepdims=True)
        scale = jnp.broadcast_to(scale, (rows, 128))
        for s in range(n_tp):
            first = lax.rem(tp_ref[0] + s, n_tp) * per

            def one(pair, _, s=s, first=first):
                at = pl.ds(pl.multiple_of(pair * 128, 128), 128)
                for m in range(n):
                    a, b = refs[m][first, :, at], refs[m][first + 1, :, at]
                    if scaled[m]:
                        a, b = a * scale, b * scale
                    even = jnp.where(low, a, pltpu.roll(b, 64, 1))
                    odd = jnp.where(low, pltpu.roll(a, 64, 1), b)
                    outs[s][2 * pair, m] = even.astype(jnp.bfloat16)
                    outs[s][2 * pair + 1, m] = odd.astype(jnp.bfloat16)
                return 0

            lax.fori_loop(0, columns // 128, one, 0, unroll=2)

    return pl.pallas_call(
        body,
        out_shape=[jax.ShapeDtypeStruct((columns // 64, n, rows, 128), jnp.bfloat16)] * n_tp,
        in_specs=[SMEM] + [VMEM] * (n + 1),
        out_specs=[VMEM] * n_tp,
        compiler_params=VMEM_LIMIT,
        name="prepare",
    )(tp_index, gain[None, :], *weights)


def placed(tp_index, blocks):
    n = len(blocks)

    def body(tp_ref, *refs):
        for s in range(n):
            refs[n][lax.rem(tp_ref[0] + (n - s), n)] = refs[s][...]

    return pl.pallas_call(
        body,
        out_shape=jax.ShapeDtypeStruct((n,) + blocks[0].shape, blocks[0].dtype),
        in_specs=[SMEM] + [VMEM] * n,
        out_specs=VMEM,
        compiler_params=VMEM_LIMIT,
        name="placed",
    )(tp_index, *blocks)


def fill(tp_ref, refs, all_ref):
    rows = refs[0].shape[0]
    for ref, ahead in zip(refs, (0, 3, 1, 2)):
        at = pl.multiple_of(lax.rem(tp_ref[0] + ahead, 4) * rows, rows)
        all_ref[pl.ds(at, rows), :] = ref[...]


def acted(tp_index, normed, gate_blocks, up_blocks, gates):
    tokens, width = normed.shape
    n = len(gate_blocks)
    units = 512
    step = tokens // 2

    def body(tp_ref, n_ref, g_ref, *refs):
        gate_ref, up_ref, out_ref = refs[-3:]
        fill(tp_ref, refs[:n], gate_ref)
        fill(tp_ref, refs[n : 2 * n], up_ref)
        low = lax.broadcasted_iota(jnp.int32, (step, 128), 1) < 64

        def one(i, _):
            rows = pl.ds(pl.multiple_of(i * step, step), step)
            for at in range(0, units, 256):
                gate, up = (
                    lax.dot_general(
                        n_ref[rows, :],
                        ref[pl.ds(at, 256), :],
                        (((1,), (1,)), ((), ())),
                        preferred_element_type=jnp.float32,
                    )
                    for ref in (gate_ref, up_ref)
                )
                for half in range(2):
                    here = slice(half * 128, (half + 1) * 128)
                    e = (at + half * 128) // 64
                    mix = jnp.where(low, g_ref[rows, e : e + 1], g_ref[rows, e + 1 : e + 2])
                    hidden = jax.nn.silu(gate[:, here]) * up[:, here] * mix
                    out_ref[rows, pl.ds(at + half * 128, 128)] = hidden.astype(jnp.bfloat16)
            return 0

        lax.fori_loop(0, 2, one, 0)

    return pl.pallas_call(
        body,
        out_shape=[jax.ShapeDtypeStruct((units, width), jnp.bfloat16)] * 2
        + [jax.ShapeDtypeStruct((tokens, units), jnp.bfloat16)],
        in_specs=[SMEM] + [VMEM] * (2 + 2 * n),
        out_specs=[VMEM] * 3,
        compiler_params=pltpu.CompilerParams(vmem_limit_bytes=28 << 20),
        name="acted",
    )(tp_index, normed, gates, *gate_blocks, *up_blocks)


def turned(block, widths):
    _, n, rows, lanes = block.shape
    step = 256 // rows
    outs = [(m, w) for m in range(n) for w in widths]

    def body(x_ref, *refs):
        for k, (m, width) in enumerate(outs):
            start = sum(w for p, w in outs[:k] if p == m) // rows

            def one(i, _, out=refs[k], m=m, start=start):
                t = x_ref[pl.ds(start + i * step, step), m].reshape(256, lanes).T
                out[:, pl.ds(pl.multiple_of(i * 256, 256), 256)] = t
                return 0

            lax.fori_loop(0, width // 256, one, 0)

    return pl.pallas_call(
        body,
        out_shape=[jax.ShapeDtypeStruct((lanes, w), block.dtype) for _, w in outs],
        in_specs=[VMEM],
        out_specs=[VMEM] * len(outs),
        compiler_params=VMEM_LIMIT,
        name="turned",
    )(block)


def gathered(name, own):

    def sent(block, by):
        return shifted(block, "tp", by)

    prev, after = sent(own, 1), sent(own, -1)
    if name in RELAYED:
        far = [sent(*((prev, 1) if RELAYED[name] > 0 else (after, -1)))]
    else:
        far = [sent(own, 2)]
    return [own, prev, after] + far


def mixed_away(tp_index, hidden, blocks):
    tokens, units = hidden.shape
    half = tokens // 2
    wide = blocks[0].shape[1]
    n = len(blocks)

    def body(tp_ref, h_ref, *refs):
        all_ref, away_ref = refs[n:]
        fill(tp_ref, refs[:n], all_ref)

        def one(i, _):
            at = pl.ds(pl.multiple_of(i * 256, 256), 256)
            part = jnp.dot(h_ref[half:], all_ref[:, at], preferred_element_type=jnp.float32)
            away_ref[:, at] = part.astype(jnp.bfloat16)
            return 0

        lax.fori_loop(0, wide // 256, one, 0)

    return pl.pallas_call(
        body,
        out_shape=[
            jax.ShapeDtypeStruct((units, wide), jnp.bfloat16),
            jax.ShapeDtypeStruct((half, wide), jnp.bfloat16),
        ],
        in_specs=[SMEM] + [VMEM] * (n + 1),
        out_specs=[VMEM] * 2,
        compiler_params=VMEM_LIMIT,
        name="mixed_away",
    )(tp_index, hidden, *blocks)


def mixed_here(hidden, down, arrived, n_x):
    half, wide = arrived.shape
    rows = half // n_x

    def body(h_ref, d_ref, r_ref, *outs):
        def one(i, _):
            at = pl.ds(pl.multiple_of(i * 256, 256), 256)
            part = jnp.dot(h_ref[:half], d_ref[:, at], preferred_element_type=jnp.float32)
            part = part + r_ref[:, at].astype(jnp.float32)
            for x in range(n_x):
                outs[x][:, at] = part[x * rows : (x + 1) * rows].astype(outs[x].dtype)
            return 0

        lax.fori_loop(0, wide // 256, one, 0)

    return pl.pallas_call(
        body,
        out_shape=[
            jax.ShapeDtypeStruct((rows, wide), jnp.bfloat16 if x else jnp.float32)
            for x in range(n_x)
        ],
        in_specs=[VMEM] * 3,
        out_specs=[VMEM] * n_x,
        compiler_params=VMEM_LIMIT,
        name="mixed_here",
    )(hidden, down, arrived)


def folded(parts, n_z):
    widths = [p[0].shape[1] for p in parts]
    count = parts[0][0].shape[0]
    width = sum(widths)
    rows, half = count // n_z, width // 2
    flat = [a for p in parts for a in p]
    per = len(parts[0])

    def body(*refs):
        outs, total = refs[len(flat) : -1], refs[-1]
        start = 0
        for c, wide in enumerate(widths):
            part = refs[c * per][...]
            for i in range(1, per):
                part = part + refs[c * per + i][...].astype(jnp.float32)
            total[:, pl.ds(start, wide)] = part
            start += wide
        for z in range(n_z):
            at = pl.ds(z * rows, rows)
            piece = jnp.concatenate([total[at, :half], total[at, half:]], axis=0)
            outs[z][...] = piece.astype(outs[z].dtype)

    return pl.pallas_call(
        body,
        out_shape=[
            jax.ShapeDtypeStruct((2 * rows, half), jnp.bfloat16 if z else jnp.float32)
            for z in range(n_z)
        ],
        in_specs=[VMEM] * len(flat),
        out_specs=[VMEM] * n_z,
        scratch_shapes=[pltpu.VMEM((count, width), jnp.float32)],
        compiler_params=VMEM_LIMIT,
        name="folded",
    )(*flat)


def finished(pieces):
    rows, half = pieces[0].shape

    def body(*refs):
        total = refs[0][...]
        for r in refs[1:-1]:
            total = total + r[...].astype(jnp.float32)
        refs[-1][:, :half] = total[: rows // 2].astype(jnp.bfloat16)
        refs[-1][:, half:] = total[rows // 2 :].astype(jnp.bfloat16)

    return pl.pallas_call(
        body,
        out_shape=jax.ShapeDtypeStruct((rows // 2, 2 * half), jnp.bfloat16),
        in_specs=[VMEM] * len(pieces),
        out_specs=VMEM,
        compiler_params=VMEM_LIMIT,
        name="finished",
    )(*pieces)


def side_by_side(parts):
    rows = parts[0].shape[0]
    widths = [p.shape[1] for p in parts]

    def body(*refs):
        for i, ref in enumerate(refs[:-1]):
            refs[-1][:, pl.ds(sum(widths[:i]), widths[i])] = ref[...]

    return pl.pallas_call(
        body,
        out_shape=jax.ShapeDtypeStruct((rows, sum(widths)), parts[0].dtype),
        in_specs=[VMEM] * len(parts),
        out_specs=VMEM,
        compiler_params=VMEM_LIMIT,
        name="side_by_side",
    )(*parts)


def local(tokens, norm_gain, gate_weight, up_weight, down_weight, expert_ids, expert_mix):
    tp = lax.axis_index("tp").astype(jnp.int32)
    tp_index = tp.reshape(1)
    n_tp = lax.axis_size("tp")

    def handed(weights, scaled):
        blocks = prepare(tp_index, norm_gain, weights, scaled)
        arrived = [blocks[0]]
        for s in range(1, n_tp):
            arrived.append(shifted(blocks[s], "tp", s))
        columns = placed(tp_index, arrived)
        columns = columns.reshape((-1,) + columns.shape[2:])
        return lax.all_to_all(columns, FS, split_axis=0, concat_axis=0, tiled=True)

    block_a = handed((gate_weight, up_weight), (True, True))
    block_d = handed((down_weight,), (False,))
    gate_own, up_own = turned(block_a, (tokens.shape[2],))
    down_own = turned(block_d, D_WIDTHS)
    gate_pieces = gathered("g", gate_own)
    up_pieces = gathered("u", up_own)
    down_pieces = [gathered(f"d{c}", own) for c, own in enumerate(down_own)]

    width = tokens.shape[2]
    count = tokens.shape[0]
    n_z, n_x, n_c = (lax.axis_size(a) for a in FS)
    own_rows = count // (n_z * n_x * n_c)
    row = jnp.arange(count, dtype=jnp.int32)
    c_at = (row // (count // n_c) + lax.axis_index("fs_2")) % n_c
    x_at = (row // (count // n_c // n_x) + lax.axis_index("fs_1")) % n_x
    z_at = (row // own_rows + lax.axis_index("fs_0")) % n_z
    source = ((z_at * n_x + x_at) * n_c + c_at) * own_rows + row % own_rows
    pick = source[:, None] == row[None, :]

    token_rows = tokens.reshape(count, width).astype(jnp.float32)
    row_mean = jnp.mean(token_rows, axis=1, keepdims=True)
    centered = token_rows - row_mean
    variance = jnp.mean(centered * centered, axis=1, keepdims=True)
    normed = (centered * lax.rsqrt(variance + norm_eps)).astype(jnp.bfloat16)
    normed = jnp.dot(pick.astype(jnp.bfloat16), normed, preferred_element_type=jnp.float32)
    normed = normed.astype(jnp.bfloat16)
    route_ids = expert_ids.reshape(-1, 2)
    route_mix = expert_mix.reshape(-1, 2)
    experts = gate_weight.shape[0]
    expert_iota = jnp.arange(experts, dtype=jnp.int32)
    expert_gates = jnp.sum(
        (route_ids[:, :, None] == expert_iota[None, None, :]).astype(jnp.float32)
        * route_mix[:, :, None],
        axis=1,
    )
    expert_gates = jnp.dot(pick.astype(jnp.float32), expert_gates, precision=lax.Precision.HIGHEST)

    gate_all, up_all, hidden = acted(tp_index, normed, gate_pieces, up_pieces, expert_gates)
    units = up_all.shape[0] // experts

    down_parts, summed = [], []
    for pieces in down_pieces:
        down_c, away = mixed_away(tp_index, hidden, pieces)
        down_parts.append(down_c)
        away = shifted(away, "fs_2", 1)
        blocks = list(mixed_here(hidden, down_c, away, n_x))
        for s in range(1, n_x):
            blocks[s] = shifted(blocks[s], "fs_1", s)
        summed.append(blocks)
    pieces = list(folded(summed, n_z))
    for s in range(1, n_z):
        pieces[s] = shifted(pieces[s], "fs_0", s)
    mixed = finished(pieces)[:, None, :]
    down_all = side_by_side(down_parts)

    def as_served(a):
        return jnp.transpose(a.reshape(experts, units, width), (0, 2, 1))

    return (as_served(gate_all), as_served(up_all), as_served(down_all), mixed)


def solution(mesh):
    finer = Mesh(mesh.devices.reshape(8, 4, 2, mesh.shape["tp"]), ("fs_0", "fs_1", "fs_2", "tp"))
    placed_as = (
        P(None, "tp", None),
        P(FS),
        P(None, FS, "tp"),
        P(None, FS, "tp"),
        P(None, FS, "tp"),
        P(None, "tp", None),
        P(None, "tp", None),
    )
    return jax.shard_map(
        local,
        mesh=finer,
        in_specs=placed_as,
        out_specs=(P(None, None, FS), P(None, None, FS), P(None, None, FS), P(FS, "tp", None)),
        check_vma=False,
    )
```
